32 devices in a mesh: sp: 8 (over z, x), tp: 4 (over y, core).
Axes of the slice: x: 2, y: 2, z: 4, core: 2. Of those that a mesh axis runs over, the one named last changes fastest.
Arguments:
- layer_input: bfloat16 [8, 4096, 2048], P(None, ('sp', 'tp')), may hold values from -6 to 6
- norm_gain: bfloat16 [2048], replicated, may hold values from 0.099609375 to 1.8984375
- key_weight: bfloat16 [2048, 1024], replicated, may hold values from -0.125 to 0.125
- value_weight: bfloat16 [2048, 1024], replicated, may hold values from -0.125 to 0.125
- new_query: bfloat16 [8, 1024], P('sp', 'tp'), may hold values from -12 to 12
- score_offset: float32 [8], replicated, may hold values from -10 to -3.5
Outputs:
- key_cache: bfloat16 [8, 4096, 1024], P('sp', None, 'tp')
- value_cache: bfloat16 [8, 4096, 1024], P('sp', None, 'tp')
- first_read: float32 [8, 1024], P('sp', 'tp')
The draws below stay inside these ranges and needn't reach their ends.
All inputs are finite; a program needn't handle non-finite values.
Results may differ from the reference program's by a relative error of at most 0.0082.
Values may be sent and summed in bfloat16 or wider, within the bound.
A program may use at most 128 MiB of HBM per device.

```python
import jax
import jax.numpy as jnp
from jax import lax

D = 2048
HEADS = 8
HEAD_DIM = 128
SEQS = 8
LENGTH = 4096


def draw_score_offset(key, part):
    return jax.random.uniform(key, (HEADS,), jnp.float32, -10.0, -3.5)


def steps_of(own_key, extent, cuts, least, top_value):
    def one(position, shards_of):
        heights = jax.random.uniform(jax.random.fold_in(jax.random.fold_in(own_key, 6), position), (shards_of,), jnp.float32, least / len(cuts), top_value / len(cuts))
        return jnp.repeat(jnp.exp(heights), extent[position] // shards_of).reshape((-1,) + (1,) * (len(extent) - position - 1))

    factor_of = one(*cuts[0])
    for cut in cuts[1:]:
        factor_of = factor_of * one(*cut)
    return factor_of


def gaussian(own_key, shape, scale, most, pieces=(), kind=jnp.bfloat16):
    array = jax.random.normal(own_key, shape, jnp.float32) * scale
    if len(pieces) > 0:
        array = steps_of(own_key, shape, pieces, -0.22, 0.18) * array
    return jnp.clip(array, min=-most, max=most).astype(kind)


def setup_inputs(seed: int = 0) -> dict:
    arg_keys = jax.random.split(jax.random.key(seed), 7)
    layer_input = gaussian(arg_keys[0], (SEQS, LENGTH, D), 1.0, 6.0, ((1, 32),))
    norm_gain = jnp.clip(1.0 + 0.18 * jax.random.normal(arg_keys[1], (D,), jnp.float32), 0.099609375, 1.8984375).astype(jnp.bfloat16)
    key_weight = gaussian(arg_keys[2], (D, HEADS * HEAD_DIM), D ** -0.5, 0.125)
    value_weight = gaussian(arg_keys[3], (D, HEADS * HEAD_DIM), D ** -0.5, 0.125)
    new_query = gaussian(arg_keys[4], (SEQS, HEADS * HEAD_DIM), 2.0, 12.0, ((0, 8), (1, 4)))
    score_offset = draw_score_offset(jax.random.fold_in(arg_keys[6], 71), 0)
    return {"layer_input": layer_input, "norm_gain": norm_gain, "key_weight": key_weight, "value_weight": value_weight, "new_query": new_query, "score_offset": score_offset}


norm_epsilon = 1e-06

def reference(layer_input, norm_gain, key_weight, value_weight, new_query, score_offset):

    def project(rows):
        wide = rows.astype(jnp.float32)
        normed = (wide * lax.rsqrt(lax.optimization_barrier(jnp.mean(wide * wide, axis=-1, keepdims=True)) + norm_epsilon) * norm_gain.astype(jnp.float32)).astype(jnp.bfloat16)
        keys = jnp.dot(normed, key_weight, preferred_element_type=jnp.float32).astype(jnp.bfloat16)
        values = jnp.dot(normed, value_weight, preferred_element_type=jnp.float32).astype(jnp.bfloat16)
        return (keys, values)
    key_cache, value_cache = lax.map(project, layer_input)
    query_heads = new_query.reshape(SEQS, HEADS, HEAD_DIM).astype(jnp.float32)
    key_heads = key_cache.reshape(SEQS, LENGTH, HEADS, HEAD_DIM).astype(jnp.float32)
    value_heads = value_cache.reshape(SEQS, LENGTH, HEADS, HEAD_DIM).astype(jnp.float32)
    scores = jnp.einsum('shd,sphd->shp', query_heads, key_heads, precision=lax.Precision.HIGHEST)
    scores = scores * HEAD_DIM ** (-0.5) + score_offset[None, :, None]
    log_rest = jax.nn.log_sigmoid(-scores)
    later = lax.cumsum(log_rest, axis=2, reverse=True) - log_rest
    weights = jnp.exp(jax.nn.log_sigmoid(scores) + later).astype(jnp.bfloat16)
    reading = jnp.einsum('shp,sphd->shd', weights.astype(jnp.float32), value_heads, precision=lax.Precision.HIGHEST)
    first_read = reading * lax.rsqrt(lax.optimization_barrier(jnp.mean(reading * reading, axis=-1, keepdims=True)) + norm_epsilon)
    return (key_cache, value_cache, first_read.reshape(SEQS, HEADS * HEAD_DIM))
```

```python
import functools

import jax
import jax.numpy as jnp
from jax import lax
from jax.experimental import pallas as pl
from jax.experimental.pallas import tpu as pltpu
from jax.sharding import PartitionSpec as P

norm_epsilon = 1e-06
MESH = pl.DeviceIdType.MESH
NORM_ROWS = 16


def exchange_kernel(
    seqs,
    groups,
    local_heads,
    x_hbm,
    gain_ref,
    key_w_hbm,
    value_w_hbm,
    query_ref,
    offset_ref,
    key_out,
    value_out,
    read_ref,
    x_buf,
    normed,
    key_w,
    value_w,
    outgoing,
    arrived,
    group_read,
    group_rest,
    x_sem,
    w_sem,
    send_sem,
    recv_sem,
    out_sem,
):
    positions = x_buf.shape[1]
    width = x_buf.shape[2]
    columns = query_ref.shape[1]
    head_dim = columns // local_heads
    span = groups * positions
    pad = group_read.shape[1]
    my_seq = lax.axis_index("sp")
    my_group = lax.axis_index("tp")
    me = my_seq * groups + my_group
    upper = (my_seq >= seqs // 2).astype(jnp.int32)
    pair = (my_seq // 2) * 2

    def seq_at(step):
        ahead = lax.rem(pair + 2 + step, seqs)
        behind = lax.rem(pair - 1 - step + 2 * seqs, seqs)
        return upper * behind + (1 - upper) * ahead

    def x_copy(step):
        seq = seq_at(step)
        return pltpu.make_async_copy(x_hbm.at[seq], x_buf.at[step], x_sem.at[step])

    def w_copy(index):
        cols = pl.ds(pl.multiple_of(index * columns, columns), columns)
        return (
            pltpu.make_async_copy(key_w_hbm.at[:, cols], key_w.at[index], w_sem.at[0, index]),
            pltpu.make_async_copy(value_w_hbm.at[:, cols], value_w.at[index], w_sem.at[1, index]),
        )

    def target(turn):
        return lax.rem(my_group + 1 + turn, groups)

    x_copy(0).start()
    for turn in range(groups):
        for copy in w_copy(target(turn)):
            copy.start()
        if turn == 0 and seqs > 1:
            x_copy(1).start()

    @pl.loop(2, seqs)
    def _(step):
        x_copy(step).start()

    barrier = pltpu.get_barrier_semaphore()

    @pl.loop(0, seqs * groups)
    def _(device):
        @pl.when(device != me)
        def _():
            pl.semaphore_signal(
                barrier,
                inc=1,
                device_id=(device // groups, lax.rem(device, groups)),
                device_id_type=MESH,
            )

    def block_rows(device):
        return pl.ds(pl.multiple_of(device * positions, positions), positions)

    def remote(seq, group):
        device = seq * groups + group
        return pltpu.make_async_remote_copy(
            src_ref=outgoing.at[seq, group],
            dst_ref=arrived.at[block_rows(me)],
            send_sem=send_sem.at[device],
            recv_sem=recv_sem.at[me],
            device_id=(seq, group),
            device_id_type=MESH,
        )

    def own():
        return pltpu.make_async_copy(
            outgoing.at[my_seq, my_group], arrived.at[block_rows(me)], recv_sem.at[me]
        )

    def launch(seq, group):
        mine = seq * groups + group == me

        @pl.when(mine)
        def _():
            own().start()

        @pl.when(jnp.logical_not(mine))
        def _():
            remote(seq, group).start()

    def norm(step):
        x_copy(step).wait()

        @pl.loop(0, positions // NORM_ROWS)
        def _(chunk):
            rows = pl.ds(pl.multiple_of(chunk * NORM_ROWS, NORM_ROWS), NORM_ROWS)
            wide = x_buf[step, rows, :].astype(jnp.float32)
            scale = lax.rsqrt(jnp.sum(wide * wide, axis=-1, keepdims=True) / width + norm_epsilon)
            normed[rows, :] = (wide * scale * gain_ref[...].astype(jnp.float32)).astype(jnp.bfloat16)

    def project(step, turn):
        seq = seq_at(step)
        group = target(turn)
        outgoing[seq, group, :, :columns] = jnp.dot(
            normed[...], key_w[group], preferred_element_type=jnp.float32
        ).astype(jnp.bfloat16)
        outgoing[seq, group, :, columns:] = jnp.dot(
            normed[...], value_w[group], preferred_element_type=jnp.float32
        ).astype(jnp.bfloat16)

    norm(0)

    @pl.loop(0, groups)
    def _(turn):
        for copy in w_copy(target(turn)):
            copy.wait()
        project(0, turn)

        @pl.when(turn == 0)
        def _():
            pl.semaphore_wait(barrier, seqs * groups - 1)

        @pl.when(turn > 0)
        def _():
            launch(seq_at(0), target(turn - 1))

    @pl.loop(1, seqs)
    def _(step):
        norm(step)
        launch(seq_at(step - 1), target(groups - 1))

        @pl.loop(0, groups)
        def _(turn):
            project(step, turn)

            @pl.when(turn > 0)
            def _():
                launch(seq_at(step), target(turn - 1))

    row = lax.broadcasted_iota(jnp.int32, (pad, columns), 0)
    col = lax.broadcasted_iota(jnp.int32, (pad, columns), 1)
    query = jnp.where(
        row == col // head_dim,
        jnp.broadcast_to(query_ref[...].astype(jnp.float32), (pad, columns)),
        0.0,
    ).astype(jnp.bfloat16)
    launch(seq_at(seqs - 1), target(groups - 1))

    score_row = lax.broadcasted_iota(jnp.int32, (pad, span), 0)
    score_col = lax.broadcasted_iota(jnp.int32, (pad, span), 1)
    offsets = jnp.zeros((pad, span), jnp.float32)
    for head in range(local_heads):
        offsets = jnp.where(score_row == head, offset_ref[my_group * local_heads + head], offsets)

    def out_copies(seq):
        rows = pl.ds(pl.multiple_of(seq * span, span), span)
        return (
            pltpu.make_async_copy(
                arrived.at[rows, pl.ds(0, columns)], key_out.at[rows], out_sem.at[0, seq]
            ),
            pltpu.make_async_copy(
                arrived.at[rows, pl.ds(columns, columns)], value_out.at[rows], out_sem.at[1, seq]
            ),
        )

    @pl.loop(0, seqs)
    def _(turn):
        seq = upper * (seqs - 1 - turn) + (1 - upper) * turn

        @pl.loop(0, groups)
        def _(group):
            device = seq * groups + group
            pltpu.make_async_copy(
                outgoing.at[seq, group], arrived.at[block_rows(device)], recv_sem.at[device]
            ).wait()

        for copy in out_copies(seq):
            copy.start()
        rows = pl.ds(pl.multiple_of(seq * span, span), span)
        scores = lax.dot_general(
            query,
            arrived[rows, :columns],
            (((1,), (1,)), ((), ())),
            preferred_element_type=jnp.float32,
        )
        scores = scores * head_dim ** (-0.5) + offsets
        soft = jnp.log1p(jnp.exp(-jnp.abs(scores)))
        rest = -jnp.maximum(scores, 0.0) - soft
        total = rest
        shift = 1
        while shift < span:
            total = total + jnp.where(
                score_col < span - shift, pltpu.roll(total, span - shift, 1), 0.0
            )
            shift *= 2
        later = total - rest
        weights = jnp.exp(jnp.minimum(scores, 0.0) - soft + later).astype(jnp.bfloat16)
        group_read[seq] = jnp.dot(
            weights, arrived[rows, columns:], preferred_element_type=jnp.float32
        )
        group_rest[seq] = jnp.broadcast_to(total[:, :1], (pad, columns))

    reading = jnp.zeros((pad, columns), jnp.float32)
    after = jnp.zeros((pad, columns), jnp.float32)
    for seq in reversed(range(seqs)):
        reading = reading + jnp.exp(after) * group_read[seq]
        after = after + group_rest[seq]
    for head in range(local_heads):
        own_cols = slice(head * head_dim, (head + 1) * head_dim)
        part = reading[head : head + 1, own_cols]
        read_ref[:, own_cols] = part * lax.rsqrt(
            jnp.mean(part * part, axis=-1, keepdims=True) + norm_epsilon
        )

    @pl.loop(0, seqs * groups)
    def _(device):
        @pl.when(device != me)
        def _():
            remote(device // groups, lax.rem(device, groups)).wait_send()

    @pl.loop(0, seqs)
    def _(seq):
        for copy in out_copies(seq):
            copy.wait()


def shards(seqs, groups, layer_input, norm_gain, key_weight, value_weight, new_query, score_offset):
    seq_count, positions, width = layer_input.shape
    columns = new_query.shape[1]
    local_heads = score_offset.shape[0] // groups
    pad = -(-local_heads // 8) * 8
    length = seqs * groups * positions
    any_space = pl.BlockSpec(memory_space=pl.ANY)
    vmem = pl.BlockSpec(memory_space=pltpu.VMEM)
    keys, values, read = pl.pallas_call(
        functools.partial(exchange_kernel, seqs, groups, local_heads),
        out_shape=(
            jax.ShapeDtypeStruct((length, columns), jnp.bfloat16),
            jax.ShapeDtypeStruct((length, columns), jnp.bfloat16),
            jax.ShapeDtypeStruct((1, columns), jnp.float32),
        ),
        in_specs=[
            any_space,
            vmem,
            any_space,
            any_space,
            vmem,
            pl.BlockSpec(memory_space=pltpu.SMEM),
        ],
        out_specs=(any_space, any_space, vmem),
        scratch_shapes=[
            pltpu.VMEM((seq_count, positions, width), jnp.bfloat16),
            pltpu.VMEM((positions, width), jnp.bfloat16),
            pltpu.VMEM((groups, width, columns), jnp.bfloat16),
            pltpu.VMEM((groups, width, columns), jnp.bfloat16),
            pltpu.VMEM((seqs, groups, positions, 2 * columns), jnp.bfloat16),
            pltpu.VMEM((length, 2 * columns), jnp.bfloat16),
            pltpu.VMEM((seqs, pad, columns), jnp.float32),
            pltpu.VMEM((seqs, pad, columns), jnp.float32),
            pltpu.SemaphoreType.DMA((seq_count,)),
            pltpu.SemaphoreType.DMA((2, groups)),
            pltpu.SemaphoreType.DMA((seqs * groups,)),
            pltpu.SemaphoreType.DMA((seqs * groups,)),
            pltpu.SemaphoreType.DMA((2, seqs)),
        ],
        compiler_params=pltpu.CompilerParams(
            collective_id=0, has_side_effects=True, vmem_limit_bytes=67043328
        ),
    )(layer_input, norm_gain.reshape(1, width), key_weight, value_weight, new_query, score_offset)
    return (keys[None], values[None], read)


def solution(mesh):
    seqs = mesh.shape["sp"]
    groups = mesh.shape["tp"]
    placed = (P(None, ("sp", "tp"), None), P(), P(), P(), P("sp", "tp"), P())
    return jax.shard_map(
        functools.partial(shards, seqs, groups),
        mesh=mesh,
        in_specs=placed,
        out_specs=(P("sp", None, "tp"), P("sp", None, "tp"), P("sp", "tp")),
        check_vma=False,
    )
```

```python
import functools

import jax
import jax.numpy as jnp
from jax import lax
from jax.experimental import pallas as pl
from jax.experimental.pallas import tpu as pltpu
from jax.sharding import PartitionSpec as P

norm_epsilon = 1e-06
MESH = pl.DeviceIdType.MESH
NORM_ROWS = 16


def exchange_kernel(
    seqs,
    groups,
    local_heads,
    x_hbm,
    gain_ref,
    key_w_hbm,
    value_w_hbm,
    query_ref,
    offset_ref,
    key_out,
    value_out,
    read_ref,
    x_buf,
    normed,
    key_w,
    value_w,
    outgoing,
    arrived,
    group_read,
    group_rest,
    x_sem,
    w_sem,
    send_sem,
    recv_sem,
    out_sem,
):
    positions = x_buf.shape[1]
    width = x_buf.shape[2]
    columns = query_ref.shape[1]
    head_dim = columns // local_heads
    span = groups * positions
    pad = group_read.shape[1]
    my_seq = lax.axis_index("sp")
    my_group = lax.axis_index("tp")
    me = my_seq * groups + my_group
    upper = (my_seq >= seqs // 2).astype(jnp.int32)
    pair = (my_seq // 2) * 2

    quad = 4 if seqs % 4 == 0 else 1

    def seq_at(step):
        if quad == 1:
            return lax.rem(my_seq + 1 + step, seqs)
        jump = 2 * (step // 4) + lax.rem(step, 2)
        side = lax.rem(my_seq + lax.rem(step // 2, 2), 2)
        ahead = lax.rem(pair + 2 + 2 * jump, seqs)
        behind = lax.rem(pair - 2 - 2 * jump + 2 * seqs, seqs)
        return upper * behind + (1 - upper) * ahead + side

    def x_copy(step):
        seq = seq_at(step)
        return pltpu.make_async_copy(x_hbm.at[seq], x_buf.at[step], x_sem.at[step])

    def w_copy(index):
        cols = pl.ds(pl.multiple_of(index * columns, columns), columns)
        return (
            pltpu.make_async_copy(key_w_hbm.at[:, cols], key_w.at[index], w_sem.at[0, index]),
            pltpu.make_async_copy(value_w_hbm.at[:, cols], value_w.at[index], w_sem.at[1, index]),
        )

    def target(turn):
        turn = lax.rem(turn + my_seq // 2, groups)
        if groups % 2 == 0:
            turn = turn // 2 + lax.rem(turn, 2) * (groups // 2)
        return lax.rem(my_group + turn, groups)

    x_copy(jnp.int32(0)).start()
    for turn in range(groups):
        for copy in w_copy(target(jnp.int32(turn))):
            copy.start()
        if turn == 0 and seqs > 1:
            x_copy(jnp.int32(1)).start()

    @pl.loop(2, seqs)
    def _(step):
        x_copy(step).start()

    barrier = pltpu.get_barrier_semaphore()

    @pl.loop(0, seqs * groups)
    def _(device):
        @pl.when(device != me)
        def _():
            pl.semaphore_signal(
                barrier,
                inc=1,
                device_id=(device // groups, lax.rem(device, groups)),
                device_id_type=MESH,
            )

    def block_rows(device):
        return pl.ds(pl.multiple_of(device * positions, positions), positions)

    def remote(seq, group):
        device = seq * groups + group
        return pltpu.make_async_remote_copy(
            src_ref=outgoing.at[seq, group],
            dst_ref=arrived.at[block_rows(me)],
            send_sem=send_sem.at[device],
            recv_sem=recv_sem.at[me],
            device_id=(seq, group),
            device_id_type=MESH,
        )

    def own():
        return pltpu.make_async_copy(
            outgoing.at[my_seq, my_group], arrived.at[block_rows(me)], recv_sem.at[me]
        )

    def launch(seq, group):
        mine = seq * groups + group == me

        @pl.when(mine)
        def _():
            own().start()

        @pl.when(jnp.logical_not(mine))
        def _():
            remote(seq, group).start()

    def norm(step):
        x_copy(step).wait()
        slot = lax.rem(step, quad)

        @pl.loop(0, positions // NORM_ROWS)
        def _(chunk):
            rows = pl.ds(pl.multiple_of(chunk * NORM_ROWS, NORM_ROWS), NORM_ROWS)
            wide = x_buf[step, rows, :].astype(jnp.float32)
            scale = lax.rsqrt(jnp.sum(wide * wide, axis=-1, keepdims=True) / width + norm_epsilon)
            gain = gain_ref[...].astype(jnp.float32).reshape(1, width)
            normed[slot, rows, :] = (wide * scale * gain).astype(jnp.bfloat16)

    def project(step, turn):
        seq = seq_at(step)
        group = target(turn)
        slot = lax.rem(step, quad)
        outgoing[seq, group, :, :columns] = jnp.dot(
            normed[slot], key_w[group], preferred_element_type=jnp.float32
        ).astype(jnp.bfloat16)
        outgoing[seq, group, :, columns:] = jnp.dot(
            normed[slot], value_w[group], preferred_element_type=jnp.float32
        ).astype(jnp.bfloat16)

    def place(index):
        phase = index // (quad * groups)
        within = lax.rem(index, quad * groups)
        return phase * quad + lax.rem(within, quad), within // quad

    def launch_at(index):
        step, turn = place(index)
        launch(seq_at(step), target(turn))

    @pl.loop(0, seqs * groups)
    def _(index):
        step, turn = place(index)

        @pl.when(turn == 0)
        def _():
            norm(step)

        @pl.when(step == 0)
        def _():
            for copy in w_copy(target(turn)):
                copy.wait()

        project(step, turn)

        @pl.when(index == 0)
        def _():
            pl.semaphore_wait(barrier, seqs * groups - 1)

        @pl.when(index > 0)
        def _():
            launch_at(index - 1)

    row = lax.broadcasted_iota(jnp.int32, (pad, columns), 0)
    col = lax.broadcasted_iota(jnp.int32, (pad, columns), 1)
    query = jnp.where(
        row == col // head_dim,
        jnp.broadcast_to(query_ref[...].astype(jnp.float32), (pad, columns)),
        0.0,
    ).astype(jnp.bfloat16)
    launch_at(jnp.int32(seqs * groups - 1))

    score_row = lax.broadcasted_iota(jnp.int32, (pad, span), 0)
    score_col = lax.broadcasted_iota(jnp.int32, (pad, span), 1)
    offsets = jnp.zeros((pad, span), jnp.float32)
    for head in range(local_heads):
        offsets = jnp.where(score_row == head, offset_ref[my_group * local_heads + head], offsets)

    def out_copies(seq):
        rows = pl.ds(pl.multiple_of(seq * span, span), span)
        return (
            pltpu.make_async_copy(
                arrived.at[rows, pl.ds(0, columns)], key_out.at[rows], out_sem.at[0, seq]
            ),
            pltpu.make_async_copy(
                arrived.at[rows, pl.ds(columns, columns)], value_out.at[rows], out_sem.at[1, seq]
            ),
        )

    @pl.loop(0, seqs)
    def _(turn):
        seq = upper * (seqs - 1 - turn) + (1 - upper) * turn

        @pl.loop(0, groups)
        def _(group):
            device = seq * groups + group
            pltpu.make_async_copy(
                outgoing.at[seq, group], arrived.at[block_rows(device)], recv_sem.at[device]
            ).wait()

        for copy in out_copies(seq):
            copy.start()
        rows = pl.ds(pl.multiple_of(seq * span, span), span)
        scores = lax.dot_general(
            query,
            arrived[rows, :columns],
            (((1,), (1,)), ((), ())),
            preferred_element_type=jnp.float32,
        )
        scores = scores * head_dim ** (-0.5) + offsets
        soft = jnp.log1p(jnp.exp(-jnp.abs(scores)))
        rest = -jnp.maximum(scores, 0.0) - soft
        total = rest
        shift = 1
        while shift < span:
            total = total + jnp.where(
                score_col < span - shift, pltpu.roll(total, span - shift, 1), 0.0
            )
            shift *= 2
        later = total - rest
        weights = jnp.exp(jnp.minimum(scores, 0.0) - soft + later).astype(jnp.bfloat16)
        group_read[seq] = jnp.dot(
            weights, arrived[rows, columns:], preferred_element_type=jnp.float32
        )
        group_rest[seq] = jnp.broadcast_to(total[:, :1], (pad, columns))

    reading = jnp.zeros((pad, columns), jnp.float32)
    after = jnp.zeros((pad, columns), jnp.float32)
    for seq in reversed(range(seqs)):
        reading = reading + jnp.exp(after) * group_read[seq]
        after = after + group_rest[seq]
    for head in range(local_heads):
        own_cols = slice(head * head_dim, (head + 1) * head_dim)
        part = reading[head : head + 1, own_cols]
        read_ref[:, own_cols] = part * lax.rsqrt(
            jnp.mean(part * part, axis=-1, keepdims=True) + norm_epsilon
        )

    @pl.loop(0, seqs * groups)
    def _(device):
        @pl.when(device != me)
        def _():
            remote(device // groups, lax.rem(device, groups)).wait_send()

    @pl.loop(0, seqs)
    def _(seq):
        for copy in out_copies(seq):
            copy.wait()


def shards(seqs, groups, layer_input, norm_gain, key_weight, value_weight, new_query, score_offset):
    seq_count, positions, width = layer_input.shape
    columns = new_query.shape[1]
    local_heads = score_offset.shape[0] // groups
    pad = -(-local_heads // 8) * 8
    length = seqs * groups * positions
    any_space = pl.BlockSpec(memory_space=pl.ANY)
    vmem = pl.BlockSpec(memory_space=pltpu.VMEM)
    keys, values, read = pl.pallas_call(
        functools.partial(exchange_kernel, seqs, groups, local_heads),
        out_shape=(
            pltpu.VMEM((length, columns), jnp.bfloat16),
            pltpu.VMEM((length, columns), jnp.bfloat16),
            jax.ShapeDtypeStruct((1, columns), jnp.float32),
        ),
        in_specs=[
            any_space,
            vmem,
            any_space,
            any_space,
            vmem,
            pl.BlockSpec(memory_space=pltpu.SMEM),
        ],
        out_specs=(vmem, vmem, vmem),
        scratch_shapes=[
            pltpu.VMEM((seq_count, positions, width), jnp.bfloat16),
            pltpu.VMEM((4 if seqs % 4 == 0 else 1, positions, width), jnp.bfloat16),
            pltpu.VMEM((groups, width, columns), jnp.bfloat16),
            pltpu.VMEM((groups, width, columns), jnp.bfloat16),
            pltpu.VMEM((seqs, groups, positions, 2 * columns), jnp.bfloat16),
            pltpu.VMEM((length, 2 * columns), jnp.bfloat16),
            pltpu.VMEM((seqs, pad, columns), jnp.float32),
            pltpu.VMEM((seqs, pad, columns), jnp.float32),
            pltpu.SemaphoreType.DMA((seq_count,)),
            pltpu.SemaphoreType.DMA((2, groups)),
            pltpu.SemaphoreType.DMA((seqs * groups,)),
            pltpu.SemaphoreType.DMA((seqs * groups,)),
            pltpu.SemaphoreType.DMA((2, seqs)),
        ],
        compiler_params=pltpu.CompilerParams(
            collective_id=0, has_side_effects=True, vmem_limit_bytes=50000000
        ),
    )(layer_input, norm_gain, key_weight, value_weight, new_query, score_offset)
    return (keys[None], values[None], read)


def solution(mesh):
    seqs = mesh.shape["sp"]
    groups = mesh.shape["tp"]
    placed = (P(None, ("sp", "tp"), None), P(), P(), P(), P("sp", "tp"), P())
    return jax.shard_map(
        functools.partial(shards, seqs, groups),
        mesh=mesh,
        in_specs=placed,
        out_specs=(P("sp", None, "tp"), P("sp", None, "tp"), P("sp", "tp")),
        check_vma=False,
    )
```
